32 devices in a mesh: sp: 8 (over z, x), tp: 4 (over y, core).
Axes of the slice: x: 2, y: 2, z: 4, core: 2. Of those that a mesh axis runs over, the one named last changes fastest.
Arguments:
- tokens: bfloat16 [4, 8192, 2048], P(None, 'sp'), may hold values from -6 to 6
- norm_gain: bfloat16 [2048], replicated, may hold values from 0.099609375 to 1.8984375
- conv_value_weight: bfloat16 [2048, 1024], P('sp', 'tp'), may hold values from -0.125 to 0.125
- conv_gate_weight: bfloat16 [2048, 1024], P('sp', 'tp'), may hold values from -0.125 to 0.125
- query_weight: bfloat16 [2048, 1024], P('sp', 'tp'), may hold values from -40 to 40
- key_weight: bfloat16 [2048, 512], P('sp', 'tp'), may hold values from -1 to 1
- value_weight: bfloat16 [2048, 512], P('sp', 'tp'), may hold values from -0.125 to 0.125
- conv_taps: bfloat16 [31, 1024], P(None, 'tp'), may hold values from -1 to 1
- conv_gain: bfloat16 [1024], P('tp'), may hold values from 0.099609375 to 1.8984375
- sink_logit: float32 [16], P('tp'), may hold values from 1 to 6
- out_conv_weight: bfloat16 [1024, 2048], P('tp', 'sp'), may hold values from -0.125 to 0.125
- out_attn_weight: bfloat16 [1024, 2048], P('tp', 'sp'), may hold values from -0.125 to 0.125
Outputs:
- mixed: bfloat16 [4, 8192, 2048], P(None, ('sp', 'tp'))
- log_total: float32 [4, 16, 8192], P(None, 'tp', 'sp')
The draws below stay inside these ranges and needn't reach their ends.
All inputs are finite; a program needn't handle non-finite values.
Results may differ from the reference program's by a relative error of at most 0.015.
Values may be sent and summed in bfloat16 or wider, within the bound.
A program may use at most 128 MiB of HBM per device.

```python
import math
import jax
import jax.numpy as jnp
from jax import lax

D = 2048
CONV_CH = 1024
HEADS = 16
KV_HEADS = 8
HEAD_DIM = 64
WINDOW = 128
CONV_K = 31
SEQS = 4
SEQ = 8192


def shared_keys(key):
    drawn = jax.random.truncated_normal(jax.random.fold_in(key, 71), -6.0, 6.0, (D, KV_HEADS * HEAD_DIM), jnp.float32)
    return drawn / jnp.sqrt(jnp.float32(D))


def draw_key_weight(key, part):
    return shared_keys(key).astype(jnp.bfloat16)


def draw_query_weight(key, part):
    drawn = jax.random.truncated_normal(jax.random.fold_in(key, 73), -6.0, 6.0, (D, HEADS * HEAD_DIM), jnp.float32)
    drawn = drawn / jnp.sqrt(jnp.float32(D))
    return drawn.astype(jnp.bfloat16)


def levels(stream_key, shape, split, smallest, largest):
    def one(dim, shards_of):
        heights = jax.random.uniform(jax.random.fold_in(jax.random.fold_in(stream_key, 6), dim), (shards_of,), jnp.float32, smallest / len(split), largest / len(split))
        return jnp.repeat(jnp.exp(heights), shape[dim] // shards_of).reshape((-1,) + (1,) * (len(shape) - dim - 1))

    gain = one(*split[0])
    for cut in split[1:]:
        gain = gain * one(*cut)
    return gain


def noise(key, dims, deviation, limit, pieces=(), kind=jnp.bfloat16):
    loudness = levels(key, dims, pieces, -0.22, 0.18) if pieces else 1.0
    result = jax.random.normal(key, dims, jnp.float32) * deviation * loudness
    return jnp.minimum(jnp.maximum(result, -limit), limit).astype(kind)


def setup_inputs(seed: int = 0) -> dict:
    streams_of = jax.random.split(jax.random.key(seed), 13)
    tokens = noise(streams_of[0], (SEQS, SEQ, D), 1.0, 6.0, ((1, 8),))
    norm_gain = jnp.clip(1.0 + 0.18 * jax.random.normal(streams_of[1], (D,), jnp.float32), 0.099609375, 1.8984375).astype(jnp.bfloat16)
    conv_value_weight = noise(streams_of[2], (D, CONV_CH), D ** -0.5, 0.125, ((0, 8), (1, 4)))
    conv_gate_weight = noise(streams_of[3], (D, CONV_CH), D ** -0.5, 0.125, ((0, 8), (1, 4)))
    query_weight = draw_query_weight(jax.random.fold_in(streams_of[12], 71), 0)
    key_weight = draw_key_weight(jax.random.fold_in(streams_of[12], 71), 0)
    value_weight = noise(streams_of[6], (D, KV_HEADS * HEAD_DIM), D ** -0.5, 0.125, ((0, 8), (1, 4)))
    conv_taps = noise(streams_of[7], (CONV_K, CONV_CH), CONV_K ** -0.5, 1.0, ((1, 4),))
    conv_gain = jnp.clip(1.0 + 0.18 * jax.random.normal(streams_of[8], (CONV_CH,), jnp.float32), 0.099609375, 1.8984375).astype(jnp.bfloat16)
    sink_logit = jnp.clip(1.0 + 5.0 * jax.random.uniform(streams_of[9], (HEADS,), jnp.float32) ** levels(streams_of[9], (HEADS,), ((0, 4),), -0.2, 0.2), 1.0, 6.0)
    out_conv_weight = noise(streams_of[10], (CONV_CH, D), (CONV_CH + HEADS * HEAD_DIM) ** -0.5, 0.125, ((0, 4), (1, 8)))
    out_attn_weight = noise(streams_of[11], (HEADS * HEAD_DIM, D), (CONV_CH + HEADS * HEAD_DIM) ** -0.5, 0.125, ((0, 4), (1, 8)))
    return dict(tokens=tokens, norm_gain=norm_gain, conv_value_weight=conv_value_weight, conv_gate_weight=conv_gate_weight, query_weight=query_weight, key_weight=key_weight, value_weight=value_weight, conv_taps=conv_taps, conv_gain=conv_gain, sink_logit=sink_logit, out_conv_weight=out_conv_weight, out_attn_weight=out_attn_weight)


EPSILON = 1e-06
ROPE_BASE = 10000.0
MASK_VALUE = -1e+30

def rotate(raw, positions):
    half_dim = raw.shape[-1] // 2
    inverse = ROPE_BASE ** (-jnp.arange(half_dim, dtype=jnp.float32) / half_dim)
    angles = positions[:, None] * inverse[None, :]
    cosine = jnp.cos(angles)[None, :, None, :]
    sine = jnp.sin(angles)[None, :, None, :]
    first, second = (raw[..., :half_dim], raw[..., half_dim:])
    return jnp.concatenate([first * cosine - second * sine, first * sine + second * cosine], axis=-1)

def reference(tokens, norm_gain, conv_value_weight, conv_gate_weight, query_weight, key_weight, value_weight, conv_taps, conv_gain, sink_logit, out_conv_weight, out_attn_weight):
    seq_count, seq_len, width = tokens.shape
    floats = tokens.astype(jnp.float32)
    row_mean = floats.mean(-1, keepdims=True)
    centred = floats - row_mean
    variance = lax.optimization_barrier(jnp.mean(centred * centred, -1, keepdims=True))
    normed = (centred * lax.rsqrt(variance + EPSILON) * norm_gain.astype(jnp.float32)).astype(jnp.bfloat16)
    flat = normed.reshape(-1, width)
    conv_value = jnp.dot(flat, conv_value_weight, preferred_element_type=jnp.float32)
    conv_gate = jnp.dot(flat, conv_gate_weight, preferred_element_type=jnp.float32)
    gated = (conv_value * jax.nn.sigmoid(conv_gate)).astype(jnp.bfloat16).reshape(seq_count, seq_len, CONV_CH)
    rim = CONV_K // 2
    padded = jnp.pad(gated, ((0, 0), (rim, rim), (0, 0)))
    taps = conv_taps.astype(jnp.float32)
    filtered = jnp.zeros((seq_count, seq_len, CONV_CH), jnp.float32)
    for tap_index in range(CONV_K):
        filtered = filtered + padded[:, tap_index:tap_index + seq_len].astype(jnp.float32) * taps[tap_index]
    chan_mean = filtered.mean(-1, keepdims=True)
    chan_centred = filtered - chan_mean
    chan_var = lax.optimization_barrier(jnp.mean(chan_centred * chan_centred, -1, keepdims=True))
    conv_out = jax.nn.silu(chan_centred * lax.rsqrt(chan_var + EPSILON) * conv_gain.astype(jnp.float32))
    conv_out = conv_out.astype(jnp.bfloat16)
    group = HEADS // KV_HEADS
    positions = jnp.arange(seq_len, dtype=jnp.float32)
    query_raw = jnp.dot(flat, query_weight, preferred_element_type=jnp.float32)
    key_raw = jnp.dot(flat, key_weight, preferred_element_type=jnp.float32)
    queries = rotate(query_raw.reshape(seq_count, seq_len, HEADS, HEAD_DIM), positions).astype(jnp.bfloat16)
    queries = queries.reshape(seq_count, seq_len, KV_HEADS, group, HEAD_DIM)
    keys = rotate(key_raw.reshape(seq_count, seq_len, KV_HEADS, HEAD_DIM), positions).astype(jnp.bfloat16)
    values = jnp.dot(flat, value_weight, preferred_element_type=jnp.float32).astype(jnp.bfloat16)
    values = values.reshape(seq_count, seq_len, KV_HEADS, HEAD_DIM)
    edge = ((0, 0), (WINDOW, WINDOW), (0, 0), (0, 0))
    keys_pad = jnp.pad(keys, edge)
    values_pad = jnp.pad(values, edge)
    block_rows = math.gcd(seq_len, 512)
    span_len = block_rows + 2 * WINDOW
    score_scale = HEAD_DIM ** (-0.5)
    sink = sink_logit.astype(jnp.float32).reshape(KV_HEADS, group)[None, :, :, None]
    relative = jnp.arange(span_len)[None, :] - jnp.arange(block_rows)[:, None]
    band = (relative >= 0) & (relative <= 2 * WINDOW)

    def one_block(block):
        first_row = (block * block_rows).astype(jnp.int32)
        q_block = lax.dynamic_slice_in_dim(queries, first_row, block_rows, 1).astype(jnp.float32)
        k_block = lax.dynamic_slice_in_dim(keys_pad, first_row, span_len, 1).astype(jnp.float32)
        v_block = lax.dynamic_slice_in_dim(values_pad, first_row, span_len, 1).astype(jnp.float32)
        scores = jnp.einsum('sqkgd,spkd->skgqp', q_block, k_block) * score_scale
        key_pos = first_row - WINDOW + jnp.arange(span_len, dtype=jnp.int32)
        allowed = band & ((key_pos >= 0) & (key_pos < seq_len))[None, :]
        scores = jnp.where(allowed, scores, MASK_VALUE)
        top = jnp.maximum(scores.max(-1), sink)
        weights = jnp.exp(scores - top[..., None])
        total = weights.sum(-1) + jnp.exp(sink - top)
        probs = (weights / total[..., None]).astype(jnp.bfloat16).astype(jnp.float32)
        out = jnp.einsum('skgqp,spkd->sqkgd', probs, v_block).astype(jnp.bfloat16)
        return (out, top + jnp.log(total))
    outs, totals = lax.map(one_block, jnp.arange(seq_len // block_rows, dtype=jnp.int32))
    attn_out = jnp.moveaxis(outs, 0, 1).reshape(seq_count * seq_len, HEADS * HEAD_DIM)
    log_total = jnp.moveaxis(totals, 0, 3).reshape(seq_count, HEADS, seq_len)
    mixed = jnp.dot(conv_out.reshape(-1, CONV_CH), out_conv_weight, preferred_element_type=jnp.float32) + jnp.dot(attn_out, out_attn_weight, preferred_element_type=jnp.float32)
    return (mixed.astype(jnp.bfloat16).reshape(seq_count, seq_len, width), log_total)
```

```python
import functools
import math

import jax
import jax.numpy as jnp
import numpy as np
from jax import lax
from jax.experimental import pallas as pl
from jax.experimental.pallas import tpu as pltpu
from jax.sharding import PartitionSpec as P

HEAD_DIM = 64
WINDOW = 128
LANES = 128
EPSILON = 1e-06
ROPE_BASE = 10000.0
MASK_VALUE = -1e30
F32 = jnp.float32
BF16 = jnp.bfloat16
FINE = 32
PROJ = 1024
TOKB = 256
SLOTS = 4
PEERS = 4
MESH = pl.DeviceIdType.MESH
VMEM_LIMIT = 67043328


def cost(flops, nbytes, trans=0):
    return pl.CostEstimate(flops=flops, bytes_accessed=nbytes, transcendentals=trans)


def grid_of(size):
    nx = max(d for d in range(1, math.isqrt(size) + 1) if size % d == 0)
    return size // nx, nx


def rope_tables(tok, size):
    half = HEAD_DIM // 2
    lane = np.arange(LANES)
    inverse = np.float32(ROPE_BASE) ** (-(lane % half).astype(np.float32) / np.float32(half))
    inverse = inverse.astype(np.float32).astype(np.float64)
    fine = np.arange(FINE)[:, None] * inverse[None]
    coarse = (np.arange(size * tok // FINE) * FINE)[:, None] * inverse[None]
    sign = np.where(lane % HEAD_DIM < half, -1.0, 1.0)[None]
    parts = (np.cos(coarse), np.sin(coarse), np.cos(fine), np.sin(fine))
    return [np.asarray(p, np.float32) for p in parts], np.asarray(sign, np.float32)


def mega_kernel(dims, *refs):
    (sp, nz, nx, ny, nc, seqs, tok, tp, ch, qw, kw, taps_n, halo, group, n_conv, n_qkv) = dims
    refs = list(refs)
    (
        tok_ref, gain_ref, cc_ref, cs_ref, fc_ref, fs_ref, sign_ref, taps_ref, cg_ref, sink_ref,
    ) = refs[:10]
    at = 10
    shards = (refs[at : at + n_conv], refs[at + n_conv : at + n_conv + n_qkv])
    at += n_conv + n_qkv
    out_shards = refs[at : at + 2]
    mixed_ref, log_ref = refs[at + 2 : at + 4]
    (
        xb, normed, wc, wq, wo, gbuf, hb, ha, xf, fst, qst, kvst, kvb, kva,
        pad, kx, vt, bias, lst, xm, stage_out, cos, sin, gain, taps, gsend, gains,
        tok_sem, piece_sem, own_sem, zs, zr, ps, pr, es, er, ds, dr,
        hs, hr, a2s, a2r, a2l, gs, gr, out_sem, log_sem,
    ) = refs[at + 4 :]
    weights = (wc, wq)
    rows, width = seqs * tok, tok_ref.shape[1]
    kd = width // sp
    share = tok // tp
    step = ch + qw
    cols = wo.shape[2]
    slots, rb = xb.shape[0], xb.shape[1]
    blocks = rows // rb
    pb = math.gcd(tok, PROJ)
    me, ti = lax.axis_index("sp"), lax.axis_index("tp")
    z, x = me // nx, lax.rem(me, nx)
    y, c = ti // nc, lax.rem(ti, nc)

    def remote(src, dst, ssem, rsem, to):
        return pltpu.make_async_remote_copy(
            src_ref=src, dst_ref=dst, send_sem=ssem, recv_sem=rsem,
            device_id=to, device_id_type=MESH,
        )

    def in_piece(g):
        def ref(zz, xx):
            slot = zz * nx + xx
            return weights[g].at[pl.ds(pl.multiple_of(slot * kd, kd), kd)]
        return ref

    def out_piece(h, zz, xx, yy, core):
        n = qw if h else ch
        row = (yy * nc + core) * step + h * ch
        return wo.at[zz * nx + xx, pl.ds(pl.multiple_of(row, math.gcd(step, ch)), n)]

    def owner_z(k):
        if k == 0:
            return z
        return z - k if k < nz else z + (k - nz + 1)

    def exists(k):
        if k == 0:
            return None
        return z >= k if k < nz else z + (k - nz + 1) < nz

    def when(cond, body):
        if cond is None:
            body()
        else:
            pl.when(cond)(body)

    arrivals = 2 * nz - 1
    lanes = [("in", g, 0) for g in range(2)]
    lanes += [("conv", 0, b) for b in range(nx)]
    lanes += [("attn", 1, e) for e in range(ny)]

    def lane_piece(lane, zz, p=0):
        kind, i, off = lanes[lane]
        if kind == "in":
            return in_piece(i)(zz, lax.rem(x + nx - p, nx))
        if kind == "conv":
            return out_piece(0, zz, lax.rem(x + nx - off, nx), lax.rem(y + ny - p, ny), c)
        return out_piece(1, zz, lax.rem(x + nx - p, nx), lax.rem(y + ny - off, ny), c)

    def fan(lane):
        return ny if lanes[lane][0] == "conv" else nx

    def fan_to(lane, p):
        if lanes[lane][0] == "conv":
            return {"tp": lax.rem(y + p, ny) * nc + c}
        return {"sp": z * nx + lax.rem(x + p, nx)}

    def hop(lane, k, up):
        piece = lane_piece(lane, owner_z(k))
        d = k if k < nz else k - nz + 1
        i = 0 if up else 1
        to = me + nx if up else me - nx
        return remote(
            piece, piece, zs.at[lane, i, d], zr.at[lane, i, d], {"sp": lax.rem(to + sp, sp)}
        )

    def landed(lane, k):
        piece = lane_piece(lane, owner_z(k))
        up = k < nz
        d = (k if up else k - nz + 1) - 1
        i = 0 if up else 1
        return remote(piece, piece, zs.at[lane, i, d], zr.at[lane, i, d], {"sp": me})

    def side(lane, k, p, arrived):
        piece = lane_piece(lane, owner_z(k), p if arrived else 0)
        i = k * PEERS + p
        return remote(piece, piece, ps.at[lane, i], pr.at[lane, i], fan_to(lane, p))

    def lane_start(lane):
        for p in range(1, fan(lane)):
            side(lane, 0, p, False).start()
        when(z < nz - 1, lambda: hop(lane, 0, True).start())
        when(z > 0, lambda: hop(lane, 0, False).start())

    def lane_poll(lane, d):
        for k in (d, nz - 1 + d):
            def body(k=k):
                landed(lane, k).wait_recv()
                if k < nz:
                    when(z < nz - 1, lambda: hop(lane, k, True).start())
                else:
                    when(z > 0, lambda: hop(lane, k, False).start())
                for p in range(1, fan(lane)):
                    side(lane, k, p, False).start()
            when(exists(k), body)

    def lane_settle(lane):
        for k in range(arrivals):
            def body(k=k):
                for p in range(1, fan(lane)):
                    side(lane, k, p, True).wait_recv()
            when(exists(k), body)

    def lane_drain(lane):
        for k in range(arrivals):
            def body(k=k):
                for p in range(1, fan(lane)):
                    side(lane, k, p, False).wait_send()
                if k < nz:
                    when(z < nz - 1, lambda: hop(lane, k, True).wait_send())
                if k == 0 or k >= nz:
                    when(z > 0, lambda: hop(lane, k, False).wait_send())
            when(exists(k), body)

    def exchange(h, p, arrived):
        if h == 0:
            piece = out_piece(0, z, lax.rem(x + nx - p, nx) if arrived else x, y, c)
            to = {"sp": z * nx + lax.rem(x + p, nx)}
        else:
            piece = out_piece(1, z, x, lax.rem(y + ny - p, ny) if arrived else y, c)
            to = {"tp": lax.rem(y + p, ny) * nc + c}
        return remote(piece, piece, es.at[h, p], er.at[h, p], to)

    def partner(lane, k, p, arrived):
        kind, h, off = lanes[lane]
        xx = lax.rem(x + nx - (off if h == 0 else p), nx)
        yy = lax.rem(y + ny - (p if h == 0 else off), ny)
        core = nc - 1 - c if arrived else c
        piece = out_piece(h, owner_z(k), xx, yy, core)
        i = k * PEERS + p
        return remote(piece, piece, ds.at[lane, i], dr.at[lane, i], {"tp": y * nc + nc - 1 - c})

    def partner_all(act, ks):
        if nc == 1:
            return
        for lane in range(2, len(lanes)):
            for k in ks:
                def body(lane=lane, k=k):
                    for p in range(fan(lane)):
                        act(lane, k, p)
                when(exists(k), body)

    def piece_copies(g):
        copies, col = [], 0
        for i, piece in enumerate(shards[g]):
            n = piece.shape[1]
            dst = weights[g].at[pl.ds(pl.multiple_of(me * kd, kd), kd), pl.ds(col, n)]
            copies.append(pltpu.make_async_copy(piece, dst, piece_sem.at[g, i]))
            col += n
        return copies

    def own_out(h):
        return pltpu.make_async_copy(out_shards[h], out_piece(h, z, x, y, c), own_sem.at[h])

    def token_copy(i):
        slot = lax.rem(i, slots)
        r = pl.multiple_of(i * rb, rb)
        return pltpu.make_async_copy(tok_ref.at[pl.ds(r, rb)], xb.at[slot], tok_sem.at[slot])

    for copy in piece_copies(0) + piece_copies(1) + [own_out(0), own_out(1)]:
        copy.start()
    for i in range(min(slots - 1, blocks)):
        token_copy(i).start()
    barrier = pltpu.get_barrier_semaphore()
    for d in range(sp):
        for e in range(tp):
            if d or e:
                to = {"sp": lax.rem(me + d, sp), "tp": lax.rem(ti + e, tp)}
                pl.semaphore_signal(barrier, inc=1, device_id=to, device_id_type=MESH)
    pl.semaphore_wait(barrier, sp * tp - 1)
    for copy in piece_copies(0):
        copy.wait()
    lane_start(0)
    for copy in piece_copies(1) + [own_out(0), own_out(1)]:
        copy.wait()
    for p in range(1, ny):
        exchange(1, p, False).start()

    gain[...] = gain_ref[...].astype(F32)
    taps[...] = taps_ref[...].astype(F32)
    gsend[...] = jnp.broadcast_to(cg_ref[...].astype(F32), gsend.shape)
    gains[ti] = jnp.broadcast_to(cg_ref[...].astype(F32), gsend.shape)
    coarse = tok // FINE
    first = pl.multiple_of(me * coarse, coarse)

    def table(i, carry):
        c1, s1 = cc_ref[pl.ds(first + i, 1)], cs_ref[pl.ds(first + i, 1)]
        c2, s2 = fc_ref[...], fs_ref[...]
        dest = pl.ds(pl.multiple_of(i * FINE, FINE), FINE)
        cos[dest] = c1 * c2 - s1 * s2
        sin[dest] = (s1 * c2 + c1 * s2) * sign_ref[...]
        return carry

    lax.fori_loop(0, coarse, table, 0)

    chunks = width // LANES
    tile = math.gcd(rb, 128)

    def norm_block(i, carry):
        @pl.when(i + slots - 1 < blocks)
        def _():
            token_copy(i + slots - 1).start()

        token_copy(i).wait()
        slot = lax.rem(i, slots)
        for t in range(rb // tile):
            def part(c):
                return xb[slot, t * tile : (t + 1) * tile, c * LANES : (c + 1) * LANES].astype(F32)

            total = part(0)
            for k in range(1, chunks):
                total = total + part(k)
            mean = jnp.sum(total, -1, keepdims=True) * (1.0 / width)
            total = None
            for k in range(chunks):
                d = part(k) - mean
                total = d * d if total is None else total + d * d
            inv = lax.rsqrt(jnp.sum(total, -1, keepdims=True) * (1.0 / width) + EPSILON)
            dest = pl.ds(pl.multiple_of(i * rb + t * tile, tile), tile)
            for k in range(chunks):
                col = k * LANES
                v = (part(k) - mean) * inv * gain[:, col : col + LANES]
                normed[dest, col : col + LANES] = v.astype(BF16)
        return carry

    def project(g, finish):
        def body(i, carry):
            r = pl.ds(pl.multiple_of(i * pb, pb), pb)
            finish(i, jnp.dot(normed[r], weights[g][...], preferred_element_type=F32))
            return carry

        lax.fori_loop(0, rows // pb, body, 0)

    per_seq = tok // pb

    def finish_gated(i, v):
        r = pl.ds(pl.multiple_of(lax.rem(i, per_seq) * pb, pb), pb)
        gbuf[i // per_seq, r] = (v[:, :ch] * jax.nn.sigmoid(v[:, ch:])).astype(BF16)

    def finish_qkv(i, v):
        s = i // per_seq
        r = pl.ds(pl.multiple_of(lax.rem(i, per_seq) * pb, pb), pb)
        co, si = cos[r], sin[r]
        lane = lax.broadcasted_iota(jnp.int32, (pb, LANES), 1)
        low = lax.rem(lane, HEAD_DIM) < HEAD_DIM // 2
        half = HEAD_DIM // 2
        for col in range(0, v.shape[1], LANES):
            part = v[:, col : col + LANES]
            if col < qw + kw:
                a, b = co, si
                if col + LANES > qw + kw:
                    turned = lane + col < qw + kw
                    a, b = jnp.where(turned, a, 1.0), jnp.where(turned, b, 0.0)
                swap = jnp.where(
                    low, pltpu.roll(part, LANES - half, 1), pltpu.roll(part, half, 1)
                )
                part = part * a + swap * b
            if col < qw:
                qst[s, r, col : col + LANES] = (part * HEAD_DIM ** (-0.5)).astype(BF16)
            else:
                kvst[s, r, col - qw : col - qw + LANES] = part.astype(BF16)

    def halo_copy(pair, up):
        buf, before, after = ((gbuf, hb, ha), (kvst, kvb, kva))[pair]
        n = before.shape[1]
        src = buf.at[:, pl.ds(tok - n, n)] if up else buf.at[:, pl.ds(0, n)]
        dst = before if up else after
        k = 0 if up else 1
        to = {"sp": lax.rem(me + 1, sp) if up else lax.rem(me + sp - 1, sp)}
        return remote(src, dst, hs.at[pair, k], hr.at[pair, k], to)

    def halo_start(pair):
        when(me < sp - 1, lambda: halo_copy(pair, True).start())
        when(me > 0, lambda: halo_copy(pair, False).start())

    def halo_wait(pair):
        before, after = ((hb, ha), (kvb, kva))[pair]

        def clear(ref):
            ref[...] = jnp.zeros_like(ref)

        when(me > 0, lambda: halo_copy(pair, True).wait_recv())
        when(me == 0, lambda: clear(before))
        when(me < sp - 1, lambda: halo_copy(pair, False).wait_recv())
        when(me == sp - 1, lambda: clear(after))

    def halo_drain(pair):
        when(me < sp - 1, lambda: halo_copy(pair, True).wait_send())
        when(me > 0, lambda: halo_copy(pair, False).wait_send())

    def token_rows(s):
        return pl.ds(pl.multiple_of(s * share, share), share)

    def scatter(b, s, e, landing):
        other = lax.rem(ti + tp - e, tp) if landing else lax.rem(ti + e, tp)
        owner = other if landing else ti
        to = ti if landing else other
        if b:
            src = gbuf.at[s, pl.ds(pl.multiple_of(to * share, share), share)]
        else:
            src = fst.at[to, s]
        col = pl.multiple_of(owner * step + b * ch, LANES)
        dst = xm.at[token_rows(s), pl.ds(col, qw if b else ch)]
        if e == 0:
            return pltpu.make_async_copy(src, dst, a2l.at[b, s])
        return remote(src, dst, a2s.at[b, s, e], a2r.at[b, s, e], {"tp": other})

    def scatter_start(b, s):
        for e in range(tp):
            scatter(b, s, e, False).start()

    def scatter_wait(b, s):
        scatter(b, s, 0, False).wait()
        for e in range(1, tp):
            scatter(b, s, e, True).wait_recv()

    lead = halo - taps_n // 2
    cr = math.gcd(share, 64)

    def depthwise(s, carry):
        xf[0:halo] = hb[s].astype(F32)
        xf[halo : halo + tok] = gbuf[s].astype(F32)
        xf[halo + tok : halo + tok + halo] = ha[s].astype(F32)

        def part_step(i, carry):
            base = pl.multiple_of(i * cr, cr)
            dest = base // share
            off = pl.multiple_of(lax.rem(base, share), cr)
            for lc in range(ch // LANES):
                ls = slice(lc * LANES, (lc + 1) * LANES)
                seg = xf[pl.ds(base, cr + 2 * halo), ls]
                total = None
                for r in range(8):
                    part = None
                    for a in range((2 * halo) // 8):
                        j = 8 * a + r - lead
                        if 0 <= j < taps_n:
                            need = cr + 8 if r else cr
                            piece = seg[8 * a : 8 * a + need] * taps[j : j + 1, ls]
                            part = piece if part is None else part + piece
                    if part is None:
                        continue
                    if r:
                        part = part[r : r + cr]
                    total = part if total is None else total + part
                fst[dest, s, pl.ds(off, cr), ls] = total.astype(BF16)
            return carry

        lax.fori_loop(0, tok // cr, part_step, 0)
        scatter_start(0, s)
        return carry

    kv2 = 2 * kw
    heads = qw // HEAD_DIM
    ar = bias.shape[2]
    span = ar + 2 * WINDOW
    length = tok + 2 * WINDOW
    vfirst = kw // LANES * LANES

    def fill_bias():
        offset = me * tok
        limit = tok * sp
        key = lax.broadcasted_iota(jnp.int32, (span, ar), 0)
        rel = key - lax.broadcasted_iota(jnp.int32, (span, ar), 1)
        band = (rel >= 0) & (rel <= 2 * WINDOW)
        for b in range(tok // ar):
            pos = key + (offset + b * ar - WINDOW)
            ok = band & (pos >= 0) & (pos < limit)
            bias[b] = jnp.where(ok, 0.0, MASK_VALUE)

    def attend(s):
        pad[0:WINDOW] = kvb[s]
        pad[WINDOW : WINDOW + tok] = kvst[s]
        pad[WINDOW + tok : length] = kva[s]
        lane = lax.broadcasted_iota(jnp.int32, (length, LANES), 1)
        for h in range(heads):
            off = (h * HEAD_DIM) % LANES
            src = (h // group) * HEAD_DIM
            chunk = src // LANES * LANES
            part = pad[:, chunk : chunk + LANES].astype(F32)
            shift = (off - src % LANES) % LANES
            if shift:
                part = pltpu.roll(part, shift, 1)
            keep = (lane >= off) & (lane < off + HEAD_DIM)
            kx[h] = jnp.where(keep, part, 0.0).astype(BF16)
        for k in range(vfirst, kv2, LANES):
            vt[k - vfirst : k - vfirst + LANES] = pad[:, k : k + LANES].astype(F32).T.astype(BF16)
        for b in range(tok // ar):
            r0 = b * ar
            for pair in range(qw // LANES):
                q = qst[s, r0 : r0 + ar, pair * LANES : (pair + 1) * LANES]
                outs = []
                for h in range(pair * 2, pair * 2 + 2):
                    sink = sink_ref[h]
                    sc = lax.dot_general(
                        kx[h, r0 : r0 + span], q, (((1,), (1,)), ((), ())),
                        preferred_element_type=F32,
                    )
                    sc = sc + bias[b]
                    top = jnp.maximum(jnp.max(sc, axis=0, keepdims=True), sink)
                    e = jnp.exp(sc - top)
                    total = jnp.sum(e, axis=0, keepdims=True) + jnp.exp(sink - top)
                    v0 = kw + (h // group) * HEAD_DIM - vfirst
                    o = jnp.dot(
                        vt[v0 : v0 + HEAD_DIM, r0 : r0 + span], e.astype(BF16),
                        preferred_element_type=F32,
                    )
                    outs.append(o / total)
                    lst[s, h : h + 1, r0 : r0 + ar] = top + jnp.log(total)
                both = jnp.concatenate(outs, axis=0).T
                gbuf[s, r0 : r0 + ar, pair * LANES : (pair + 1) * LANES] = both.astype(BF16)

    def activate(s):
        parts = [xm[token_rows(s), t * step : t * step + ch].astype(F32) for t in range(tp)]
        mean = sum(p.sum(-1, keepdims=True) for p in parts) / (tp * ch)
        parts = [p - mean for p in parts]
        var = sum((p * p).sum(-1, keepdims=True) for p in parts) / (tp * ch)
        inv = lax.rsqrt(var + EPSILON)
        for t in range(tp):
            v = parts[t] * inv * gains[t, 0:1]
            xm[token_rows(s), t * step : t * step + ch] = jax.nn.silu(v).astype(BF16)

    def gain_copy(e, landing):
        other = lax.rem(ti + tp - e, tp) if landing else lax.rem(ti + e, tp)
        dst = gains.at[other if landing else ti]
        return remote(gsend, dst, gs.at[e], gr.at[e], {"tp": other})

    assert ch == qw
    fill_bias()
    cuts = [0] + [blocks * (3 + 2 * k) // 8 for k in range(nz - 1)] + [blocks]
    cuts = [min(k, blocks) for k in cuts]
    for k in range(nz):
        lax.fori_loop(cuts[k], cuts[k + 1], norm_block, 0)
        if k < nz - 1:
            lane_poll(0, k + 1)
        if k == 0:
            for e in range(1, tp):
                gain_copy(e, False).start()
        if k == 1:
            lane_start(1)
    for p in range(1, nx):
        exchange(0, p, False).start()
    lane_poll(1, 1)
    lane_settle(0)
    project(0, finish_gated)
    halo_start(0)
    for d in range(2, nz):
        lane_poll(1, d)
    halo_wait(0)
    early = max(seqs - 1, 1)
    lax.fori_loop(0, early, depthwise, 0)
    for p in range(1, nx):
        exchange(0, p, True).wait_recv()
    for p in range(1, ny):
        exchange(1, p, True).wait_recv()
    for lane in range(2, len(lanes)):
        lane_start(lane)
    lane_settle(1)
    project(1, finish_qkv)
    halo_start(1)
    lax.fori_loop(early, seqs, depthwise, 0)
    for lane in range(2, len(lanes)):
        lane_poll(lane, 1)
    partner_all(lambda lane, k, p: None if p else partner(lane, k, p, False).start(), (0,))
    for e in range(1, tp):
        gain_copy(e, True).wait_recv()
    halo_drain(0)
    halo_wait(1)

    def attend_step(s, carry):
        attend(s)
        scatter_start(1, s)
        scatter_wait(0, s)
        activate(s)
        for d in range(2, nz):
            @pl.when(s == min(d - 2, seqs - 1))
            def _():
                for lane in range(2, len(lanes)):
                    lane_poll(lane, d)

        @pl.when(s == seqs - 2)
        def _():
            for k in range(1, arrivals):
                partner_all(lambda lane, k, p: None if p else partner(lane, k, p, False).start(), (k,))
        return carry

    lax.fori_loop(0, seqs, attend_step, 0)
    log_copy = pltpu.make_async_copy(lst, log_ref, log_sem.at[0])
    log_copy.start()
    for lane in range(2, len(lanes)):
        lane_settle(lane)
    partner_all(lambda lane, k, p: partner(lane, k, p, False).start() if p else None, range(arrivals))
    for s in range(seqs):
        scatter_wait(1, s)
    partner_all(lambda lane, k, p: partner(lane, k, p, True).wait_recv(), range(arrivals))

    def out_copy(j):
        slot = lax.rem(j, 2)
        dst = mixed_ref.at[:, :, pl.ds(pl.multiple_of(j * cols, cols), cols)]
        return pltpu.make_async_copy(stage_out.at[slot], dst, out_sem.at[slot])

    def out_step(j, carry):
        @pl.when(j >= 2)
        def _():
            out_copy(j - 2).wait()

        v = jnp.dot(xm[...], wo[j], preferred_element_type=F32).astype(BF16)
        stage_out[lax.rem(j, 2)] = v.reshape(seqs, share, cols)
        out_copy(j).start()
        return carry

    lax.fori_loop(0, sp, out_step, 0)

    for lane in range(len(lanes)):
        lane_drain(lane)
    for p in range(1, nx):
        exchange(0, p, False).wait_send()
    for p in range(1, ny):
        exchange(1, p, False).wait_send()
    partner_all(lambda lane, k, p: partner(lane, k, p, False).wait_send(), range(arrivals))
    for e in range(1, tp):
        gain_copy(e, False).wait_send()
    halo_drain(1)
    for b in range(2):
        for s in range(seqs):
            for e in range(1, tp):
                scatter(b, s, e, False).wait_send()
    log_copy.wait()
    for j in range(max(sp - 2, 0), sp):
        out_copy(j).wait()


def mega(tokens, norm_gain, taps, conv_gain, sink, conv_shards, qkv_shards, out_shards, qw, kw):
    seqs, tok, width = tokens.shape
    tp, sp = lax.axis_size("tp"), lax.axis_size("sp")
    nz, nx = grid_of(sp)
    nc = 2 if tp % 2 == 0 else 1
    ny = tp // nc
    rows = seqs * tok
    taps_n, ch = taps.shape
    kd = width // sp
    halo = -(-(taps_n // 2) // 16) * 16
    rb = math.gcd(tok, TOKB)
    share = tok // tp
    heads = qw // HEAD_DIM
    group = heads // (kw // HEAD_DIM)
    cols = out_shards[0].shape[1]
    step = ch + qw
    tables, sign = rope_tables(tok, sp)
    dims = (
        sp, nz, nx, ny, nc, seqs, tok, tp, ch, qw, kw, taps_n, halo, group,
        len(conv_shards), len(qkv_shards),
    )
    vmem = pl.BlockSpec(memory_space=pltpu.VMEM)
    hbm = pl.BlockSpec(memory_space=pl.ANY)
    n = qw + 2 * kw
    pieces = len(conv_shards) + len(qkv_shards) + 2
    ar = math.gcd(share, 256)
    span = ar + 2 * WINDOW
    length = tok + 2 * WINDOW
    vfirst = kw // LANES * LANES
    lanes = 2 + nx + ny
    dma = pltpu.SemaphoreType.DMA
    per_lane = (2 * nz - 1) * PEERS
    return pl.pallas_call(
        functools.partial(mega_kernel, dims),
        in_specs=[hbm] + [vmem] * 8 + [pl.BlockSpec(memory_space=pltpu.SMEM)] + [hbm] * pieces,
        out_specs=[hbm] * 2,
        out_shape=[
            jax.ShapeDtypeStruct((seqs, share, width), BF16),
            jax.ShapeDtypeStruct((seqs, heads, tok), F32),
        ],
        scratch_shapes=[
            pltpu.VMEM((SLOTS, rb, width), BF16),
            pltpu.VMEM((rows, width), BF16),
            pltpu.VMEM((width, 2 * ch), BF16),
            pltpu.VMEM((width, n), BF16),
            pltpu.VMEM((sp, tp * step, cols), BF16),
            pltpu.VMEM((seqs, tok, ch), BF16),
            pltpu.VMEM((seqs, halo, ch), BF16),
            pltpu.VMEM((seqs, halo, ch), BF16),
            pltpu.VMEM((tok + 2 * halo, ch), F32),
            pltpu.VMEM((tp, seqs, share, ch), BF16),
            pltpu.VMEM((seqs, tok, qw), BF16),
            pltpu.VMEM((seqs, tok, 2 * kw), BF16),
            pltpu.VMEM((seqs, WINDOW, 2 * kw), BF16),
            pltpu.VMEM((seqs, WINDOW, 2 * kw), BF16),
            pltpu.VMEM((length, 2 * kw), BF16),
            pltpu.VMEM((heads, length, LANES), BF16),
            pltpu.VMEM((2 * kw - vfirst, length), BF16),
            pltpu.VMEM((tok // ar, span, ar), F32),
            pltpu.VMEM((seqs, heads, tok), F32),
            pltpu.VMEM((seqs * share, tp * step), BF16),
            pltpu.VMEM((2, seqs, share, cols), BF16),
            pltpu.VMEM((tok, LANES), F32),
            pltpu.VMEM((tok, LANES), F32),
            pltpu.VMEM((1, width), F32),
            pltpu.VMEM((taps_n, ch), F32),
            pltpu.VMEM((8, ch), F32),
            pltpu.VMEM((tp, 8, ch), F32),
            dma((SLOTS,)),
            dma((2, max(len(conv_shards), len(qkv_shards)))),
            dma((2,)),
            dma((lanes, 2, nz)),
            dma((lanes, 2, nz)),
            dma((lanes, per_lane)),
            dma((lanes, per_lane)),
            dma((2, PEERS)),
            dma((2, PEERS)),
            dma((lanes, per_lane)),
            dma((lanes, per_lane)),
            dma((2, 2)),
            dma((2, 2)),
            dma((2, seqs, tp)),
            dma((2, seqs, tp)),
            dma((2, seqs)),
            dma((tp,)),
            dma((tp,)),
            dma((2,)),
            dma((1,)),
        ],
        compiler_params=pltpu.CompilerParams(
            vmem_limit_bytes=VMEM_LIMIT, collective_id=0, has_side_effects=True
        ),
        cost_estimate=cost(6 * rows * width * (n + 2 * ch), 4 * rows * width),
        name="layer",
    )(
        tokens.reshape(rows, width),
        norm_gain.reshape(1, width),
        *tables,
        sign,
        taps,
        conv_gain.reshape(1, ch),
        sink,
        *conv_shards,
        *qkv_shards,
        *out_shards,
    )


def on_device(
    tokens,
    norm_gain,
    conv_value_weight,
    conv_gate_weight,
    query_weight,
    key_weight,
    value_weight,
    conv_taps,
    conv_gain,
    sink_logit,
    out_conv_weight,
    out_attn_weight,
):
    qw, kw = query_weight.shape[1], key_weight.shape[1]
    qkv_shards = [query_weight, key_weight, value_weight]
    if kw % LANES:
        qkv_shards[1:] = [jnp.concatenate(qkv_shards[1:], 1)]
    mixed, log_total = mega(
        tokens,
        norm_gain,
        conv_taps,
        conv_gain,
        sink_logit,
        [conv_value_weight, conv_gate_weight],
        qkv_shards,
        [out_conv_weight, out_attn_weight],
        qw,
        kw,
    )
    return (mixed, log_total)


def solution(mesh):
    placed = (
        P(None, "sp", None),
        P(),
        P("sp", "tp"),
        P("sp", "tp"),
        P("sp", "tp"),
        P("sp", "tp"),
        P("sp", "tp"),
        P(None, "tp"),
        P("tp"),
        P("tp"),
        P("tp", "sp"),
        P("tp", "sp"),
    )
    return jax.shard_map(
        on_device,
        mesh=mesh,
        in_specs=placed,
        out_specs=(P(None, ("sp", "tp"), None), P(None, "tp", "sp")),
        check_vma=False,
    )
```

```python
import functools
import math

import jax
import jax.numpy as jnp
import numpy as np
from jax import lax
from jax.experimental import pallas as pl
from jax.experimental.pallas import tpu as pltpu
from jax.sharding import PartitionSpec as P

HEAD_DIM = 64
WINDOW = 128
LANES = 128
EPSILON = 1e-06
ROPE_BASE = 10000.0
MASK_VALUE = -1e30
F32 = jnp.float32
BF16 = jnp.bfloat16
FINE = 32
PROJ = 1024
TOKB = 256
SLOTS = 4
PEERS = 4
MESH = pl.DeviceIdType.MESH
VMEM_LIMIT = 67043328


def cost(flops, nbytes, trans=0):
    return pl.CostEstimate(flops=flops, bytes_accessed=nbytes, transcendentals=trans)


def grid_of(size):
    nx = max(d for d in range(1, math.isqrt(size) + 1) if size % d == 0)
    return size // nx, nx


def rope_tables(tok, size):
    half = HEAD_DIM // 2
    lane = np.arange(LANES)
    inverse = np.float32(ROPE_BASE) ** (-(lane % half).astype(np.float32) / np.float32(half))
    inverse = inverse.astype(np.float32).astype(np.float64)
    fine = np.arange(FINE)[:, None] * inverse[None]
    coarse = (np.arange(size * tok // FINE) * FINE)[:, None] * inverse[None]
    sign = np.where(lane % HEAD_DIM < half, -1.0, 1.0)[None]
    parts = (np.cos(coarse), np.sin(coarse), np.cos(fine), np.sin(fine))
    return [np.asarray(p, np.float32) for p in parts], np.asarray(sign, np.float32)


def mega_kernel(dims, *refs):
    (sp, nz, nx, ny, nc, seqs, tok, tp, ch, qw, kw, taps_n, halo, group, n_conv, n_qkv) = dims
    refs = list(refs)
    (
        tok_ref, gain_ref, cc_ref, cs_ref, fc_ref, fs_ref, sign_ref, taps_ref, cg_ref, sink_ref,
    ) = refs[:10]
    at = 10
    shards = (refs[at : at + n_conv], refs[at + n_conv : at + n_conv + n_qkv])
    at += n_conv + n_qkv
    out_shards = refs[at : at + 2]
    mixed_ref, log_ref = refs[at + 2 : at + 4]
    (
        xb, normed, wc, wq, wo, gbuf, hb, ha, xf, fst, qst, kvst, kvb, kva,
        pad, kx, vt, bias, lst, xm, stage_out, cos, sin, gain, taps, gsend, gains,
        tok_sem, piece_sem, own_sem, zs, zr, ps, pr, es, er, ds, dr,
        hs, hr, a2s, a2r, a2l, gs, gr, out_sem, log_sem,
    ) = refs[at + 4 :]
    weights = (wc, wq)
    rows, width = seqs * tok, tok_ref.shape[1]
    kd = width // sp
    share = tok // tp
    step = ch + qw
    cols = wo.shape[2]
    slots, rb = xb.shape[0], xb.shape[1]
    blocks = rows // rb
    pb = math.gcd(tok, PROJ)
    me, ti = lax.axis_index("sp"), lax.axis_index("tp")
    z, x = me // nx, lax.rem(me, nx)
    y, c = ti // nc, lax.rem(ti, nc)

    def remote(src, dst, ssem, rsem, to):
        return pltpu.make_async_remote_copy(
            src_ref=src, dst_ref=dst, send_sem=ssem, recv_sem=rsem,
            device_id=to, device_id_type=MESH,
        )

    def in_piece(g):
        def ref(zz, xx):
            slot = zz * nx + xx
            return weights[g].at[pl.ds(pl.multiple_of(slot * kd, kd), kd)]
        return ref

    def out_piece(h, zz, xx, yy, core):
        n = qw if h else ch
        row = (yy * nc + core) * step + h * ch
        return wo.at[zz * nx + xx, pl.ds(pl.multiple_of(row, math.gcd(step, ch)), n)]

    def owner_z(k):
        if k == 0:
            return z
        return z - k if k < nz else z + (k - nz + 1)

    def exists(k):
        if k == 0:
            return None
        return z >= k if k < nz else z + (k - nz + 1) < nz

    def when(cond, body):
        if cond is None:
            body()
        else:
            pl.when(cond)(body)

    arrivals = 2 * nz - 1
    lanes = [("in", g, 0) for g in range(2)]
    lanes += [("conv", 0, b) for b in range(nx)]
    lanes += [("attn", 1, e) for e in range(ny)]

    def lane_piece(lane, zz, p=0):
        kind, i, off = lanes[lane]
        if kind == "in":
            return in_piece(i)(zz, lax.rem(x + nx - p, nx))
        if kind == "conv":
            return out_piece(0, zz, lax.rem(x + nx - off, nx), lax.rem(y + ny - p, ny), c)
        return out_piece(1, zz, lax.rem(x + nx - p, nx), lax.rem(y + ny - off, ny), c)

    def fan(lane):
        return ny if lanes[lane][0] == "conv" else nx

    def fan_to(lane, p):
        if lanes[lane][0] == "conv":
            return {"tp": lax.rem(y + p, ny) * nc + c}
        return {"sp": z * nx + lax.rem(x + p, nx)}

    def hop(lane, k, up):
        piece = lane_piece(lane, owner_z(k))
        d = k if k < nz else k - nz + 1
        i = 0 if up else 1
        to = me + nx if up else me - nx
        return remote(
            piece, piece, zs.at[lane, i, d], zr.at[lane, i, d], {"sp": lax.rem(to + sp, sp)}
        )

    def landed(lane, k):
        piece = lane_piece(lane, owner_z(k))
        up = k < nz
        d = (k if up else k - nz + 1) - 1
        i = 0 if up else 1
        return remote(piece, piece, zs.at[lane, i, d], zr.at[lane, i, d], {"sp": me})

    def side(lane, k, p, arrived):
        piece = lane_piece(lane, owner_z(k), p if arrived else 0)
        i = k * PEERS + p
        return remote(piece, piece, ps.at[lane, i], pr.at[lane, i], fan_to(lane, p))

    def fan_start(lane):
        for p in range(1, fan(lane)):
            side(lane, 0, p, False).start()

    def hop_start(lane):
        when(z < nz - 1, lambda: hop(lane, 0, True).start())
        when(z > 0, lambda: hop(lane, 0, False).start())

    def lane_poll(lane, d):
        for k in (d, nz - 1 + d):
            def body(k=k):
                landed(lane, k).wait_recv()
                if k < nz:
                    when(z < nz - 1, lambda: hop(lane, k, True).start())
                else:
                    when(z > 0, lambda: hop(lane, k, False).start())
                for p in range(1, fan(lane)):
                    side(lane, k, p, False).start()
            when(exists(k), body)

    def lane_settle(lane):
        for k in range(arrivals):
            def body(k=k):
                for p in range(1, fan(lane)):
                    side(lane, k, p, True).wait_recv()
            when(exists(k), body)

    def lane_drain(lane):
        for k in range(arrivals):
            def body(k=k):
                for p in range(1, fan(lane)):
                    side(lane, k, p, False).wait_send()
                if k < nz:
                    when(z < nz - 1, lambda: hop(lane, k, True).wait_send())
                if k == 0 or k >= nz:
                    when(z > 0, lambda: hop(lane, k, False).wait_send())
            when(exists(k), body)

    def exchange(h, p, arrived):
        if h == 0:
            piece = out_piece(0, z, lax.rem(x + nx - p, nx) if arrived else x, y, c)
            to = {"sp": z * nx + lax.rem(x + p, nx)}
        else:
            piece = out_piece(1, z, x, lax.rem(y + ny - p, ny) if arrived else y, c)
            to = {"tp": lax.rem(y + p, ny) * nc + c}
        return remote(piece, piece, es.at[h, p], er.at[h, p], to)

    def partner(lane, k, p, arrived):
        kind, h, off = lanes[lane]
        xx = lax.rem(x + nx - (off if h == 0 else p), nx)
        yy = lax.rem(y + ny - (p if h == 0 else off), ny)
        core = nc - 1 - c if arrived else c
        piece = out_piece(h, owner_z(k), xx, yy, core)
        i = k * PEERS + p
        return remote(piece, piece, ds.at[lane, i], dr.at[lane, i], {"tp": y * nc + nc - 1 - c})

    def partner_all(act, ks):
        if nc == 1:
            return
        for lane in range(2, len(lanes)):
            for k in ks:
                def body(lane=lane, k=k):
                    for p in range(fan(lane)):
                        act(lane, k, p)
                when(exists(k), body)

    def piece_copies(g):
        copies, col = [], 0
        for i, piece in enumerate(shards[g]):
            n = piece.shape[1]
            dst = weights[g].at[pl.ds(pl.multiple_of(me * kd, kd), kd), pl.ds(col, n)]
            copies.append(pltpu.make_async_copy(piece, dst, piece_sem.at[g, i]))
            col += n
        return copies

    def own_out(h):
        return pltpu.make_async_copy(out_shards[h], out_piece(h, z, x, y, c), own_sem.at[h])

    def token_copy(i):
        slot = lax.rem(i, slots)
        r = pl.multiple_of(i * rb, rb)
        return pltpu.make_async_copy(tok_ref.at[pl.ds(r, rb)], xb.at[slot], tok_sem.at[slot])

    for copy in piece_copies(0) + piece_copies(1) + [own_out(0), own_out(1)]:
        copy.start()
    for i in range(min(slots - 1, blocks)):
        token_copy(i).start()
    barrier = pltpu.get_barrier_semaphore()
    for d in range(sp):
        for e in range(tp):
            if d or e:
                to = {"sp": lax.rem(me + d, sp), "tp": lax.rem(ti + e, tp)}
                pl.semaphore_signal(barrier, inc=1, device_id=to, device_id_type=MESH)
    pl.semaphore_wait(barrier, sp * tp - 1)
    for copy in piece_copies(0):
        copy.wait()
    fan_start(0)
    hop_start(0)
    for copy in piece_copies(1) + [own_out(0), own_out(1)]:
        copy.wait()
    for p in range(1, ny):
        exchange(1, p, False).start()

    gain[...] = gain_ref[...].astype(F32).reshape(1, width)
    taps[...] = taps_ref[...].astype(F32)
    gsend[...] = jnp.broadcast_to(cg_ref[...].astype(F32).reshape(1, ch), gsend.shape)
    gains[ti] = jnp.broadcast_to(cg_ref[...].astype(F32).reshape(1, ch), gsend.shape)
    coarse = tok // FINE
    first = pl.multiple_of(me * coarse, coarse)

    def table(i, carry):
        c1, s1 = cc_ref[pl.ds(first + i, 1)], cs_ref[pl.ds(first + i, 1)]
        c2, s2 = fc_ref[...], fs_ref[...]
        dest = pl.ds(pl.multiple_of(i * FINE, FINE), FINE)
        cos[dest] = c1 * c2 - s1 * s2
        sin[dest] = (s1 * c2 + c1 * s2) * sign_ref[...]
        return carry

    lax.fori_loop(0, coarse, table, 0)

    chunks = width // LANES
    tile = math.gcd(rb, 128)

    def norm_block(i, carry):
        @pl.when(i + slots - 1 < blocks)
        def _():
            token_copy(i + slots - 1).start()

        token_copy(i).wait()
        slot = lax.rem(i, slots)
        for t in range(rb // tile):
            def part(c):
                return xb[slot, t * tile : (t + 1) * tile, c * LANES : (c + 1) * LANES].astype(F32)

            total = part(0)
            for k in range(1, chunks):
                total = total + part(k)
            mean = jnp.sum(total, -1, keepdims=True) * (1.0 / width)
            total = None
            for k in range(chunks):
                d = part(k) - mean
                total = d * d if total is None else total + d * d
            inv = lax.rsqrt(jnp.sum(total, -1, keepdims=True) * (1.0 / width) + EPSILON)
            dest = pl.ds(pl.multiple_of(i * rb + t * tile, tile), tile)
            for k in range(chunks):
                col = k * LANES
                v = (part(k) - mean) * inv * gain[:, col : col + LANES]
                normed[dest, col : col + LANES] = v.astype(BF16)
        return carry

    per_seq = tok // pb

    def project(g, finish, polls):
        def body(i, carry):
            r = pl.ds(pl.multiple_of(i * pb, pb), pb)
            finish(i, jnp.dot(normed[r], weights[g][...], preferred_element_type=F32))
            when(lax.rem(i, per_seq) == per_seq - 1, lambda: halo_start(g, i // per_seq))
            for k, poll in enumerate(polls):
                when(i == min(k, rows // pb - 1), poll)
            return carry

        lax.fori_loop(0, rows // pb, body, 0)

    def finish_gated(i, v):
        r = pl.ds(pl.multiple_of(lax.rem(i, per_seq) * pb, pb), pb)
        gbuf[i // per_seq, r] = (v[:, :ch] * jax.nn.sigmoid(v[:, ch:])).astype(BF16)

    def finish_qkv(i, v):
        s = i // per_seq
        r = pl.ds(pl.multiple_of(lax.rem(i, per_seq) * pb, pb), pb)
        co, si = cos[r], sin[r]
        lane = lax.broadcasted_iota(jnp.int32, (pb, LANES), 1)
        low = lax.rem(lane, HEAD_DIM) < HEAD_DIM // 2
        half = HEAD_DIM // 2
        for col in range(0, v.shape[1], LANES):
            part = v[:, col : col + LANES]
            if col < qw + kw:
                a, b = co, si
                if col + LANES > qw + kw:
                    turned = lane + col < qw + kw
                    a, b = jnp.where(turned, a, 1.0), jnp.where(turned, b, 0.0)
                swap = jnp.where(
                    low, pltpu.roll(part, LANES - half, 1), pltpu.roll(part, half, 1)
                )
                part = part * a + swap * b
            if col < qw:
                qst[s, r, col : col + LANES] = (part * HEAD_DIM ** (-0.5)).astype(BF16)
            else:
                kvst[s, r, col - qw : col - qw + LANES] = part.astype(BF16)

    def halo_copy(pair, up, s):
        buf, before, after = ((gbuf, hb, ha), (kvst, kvb, kva))[pair]
        n = before.shape[1]
        src = buf.at[s, pl.ds(tok - n, n)] if up else buf.at[s, pl.ds(0, n)]
        dst = (before if up else after).at[s]
        k = 0 if up else 1
        to = {"sp": lax.rem(me + 1, sp) if up else lax.rem(me + sp - 1, sp)}
        return remote(src, dst, hs.at[pair, k, s], hr.at[pair, k, s], to)

    def halo_start(pair, s):
        when(me < sp - 1, lambda: halo_copy(pair, True, s).start())
        when(me > 0, lambda: halo_copy(pair, False, s).start())

    def halo_clear():
        def clear(refs):
            for ref in refs:
                ref[...] = jnp.zeros_like(ref)

        when(me == 0, lambda: clear((hb, kvb)))
        when(me == sp - 1, lambda: clear((ha, kva)))

    def halo_wait(pair, s):
        when(me > 0, lambda: halo_copy(pair, True, s).wait_recv())
        when(me < sp - 1, lambda: halo_copy(pair, False, s).wait_recv())

    def halo_drain(pair, s):
        when(me < sp - 1, lambda: halo_copy(pair, True, s).wait_send())
        when(me > 0, lambda: halo_copy(pair, False, s).wait_send())

    def token_rows(s):
        return pl.ds(pl.multiple_of(s * share, share), share)

    def scatter(b, s, e, landing):
        other = lax.rem(ti + tp - e, tp) if landing else lax.rem(ti + e, tp)
        owner = other if landing else ti
        to = ti if landing else other
        if b:
            src = gbuf.at[s, pl.ds(pl.multiple_of(to * share, share), share)]
        else:
            src = fst.at[to, s]
        col = pl.multiple_of(owner * step + b * ch, LANES)
        dst = xm.at[token_rows(s), pl.ds(col, qw if b else ch)]
        if e == 0:
            return pltpu.make_async_copy(src, dst, a2l.at[b, s])
        return remote(src, dst, a2s.at[b, s, e], a2r.at[b, s, e], {"tp": other})

    def scatter_start(b, s):
        for e in range(tp):
            scatter(b, s, e, False).start()

    def scatter_wait(b, s):
        scatter(b, s, 0, False).wait()
        for e in range(1, tp):
            scatter(b, s, e, True).wait_recv()

    lead = halo - taps_n // 2
    cr = math.gcd(share, 64)

    def depthwise(s, carry):
        halo_wait(0, s)
        xf[0:halo] = hb[s].astype(F32)
        xf[halo : halo + tok] = gbuf[s].astype(F32)
        xf[halo + tok : halo + tok + halo] = ha[s].astype(F32)

        def part_step(i, carry):
            base = pl.multiple_of(i * cr, cr)
            dest = base // share
            off = pl.multiple_of(lax.rem(base, share), cr)
            for lc in range(ch // LANES):
                ls = slice(lc * LANES, (lc + 1) * LANES)
                seg = xf[pl.ds(base, cr + 2 * halo), ls]
                total = None
                for r in range(8):
                    part = None
                    for a in range((2 * halo) // 8):
                        j = 8 * a + r - lead
                        if 0 <= j < taps_n:
                            need = cr + 8 if r else cr
                            piece = seg[8 * a : 8 * a + need] * taps[j : j + 1, ls]
                            part = piece if part is None else part + piece
                    if part is None:
                        continue
                    if r:
                        part = part[r : r + cr]
                    total = part if total is None else total + part
                fst[dest, s, pl.ds(off, cr), ls] = total.astype(BF16)
            return carry

        lax.fori_loop(0, tok // cr, part_step, 0)
        scatter_start(0, s)
        return carry

    kv2 = 2 * kw
    heads = qw // HEAD_DIM
    ar = bias.shape[2]
    span = ar + 2 * WINDOW
    length = tok + 2 * WINDOW
    vfirst = kw // LANES * LANES

    def fill_bias():
        offset = me * tok
        limit = tok * sp
        key = lax.broadcasted_iota(jnp.int32, (span, ar), 0)
        rel = key - lax.broadcasted_iota(jnp.int32, (span, ar), 1)
        band = (rel >= 0) & (rel <= 2 * WINDOW)
        for b in range(tok // ar):
            pos = key + (offset + b * ar - WINDOW)
            ok = band & (pos >= 0) & (pos < limit)
            bias[b] = jnp.where(ok, 0.0, MASK_VALUE)

    def attend(s):
        pad[0:WINDOW] = kvb[s]
        pad[WINDOW : WINDOW + tok] = kvst[s]
        pad[WINDOW + tok : length] = kva[s]
        lane = lax.broadcasted_iota(jnp.int32, (length, LANES), 1)
        for h in range(heads):
            off = (h * HEAD_DIM) % LANES
            src = (h // group) * HEAD_DIM
            chunk = src // LANES * LANES
            part = pad[:, chunk : chunk + LANES].astype(F32)
            shift = (off - src % LANES) % LANES
            if shift:
                part = pltpu.roll(part, shift, 1)
            keep = (lane >= off) & (lane < off + HEAD_DIM)
            kx[h] = jnp.where(keep, part, 0.0).astype(BF16)
        for k in range(vfirst, kv2, LANES):
            vt[k - vfirst : k - vfirst + LANES] = pad[:, k : k + LANES].astype(F32).T.astype(BF16)
        for b in range(tok // ar):
            r0 = b * ar
            for pair in range(qw // LANES):
                q = qst[s, r0 : r0 + ar, pair * LANES : (pair + 1) * LANES]
                outs = []
                for h in range(pair * 2, pair * 2 + 2):
                    sink = sink_ref[h]
                    sc = lax.dot_general(
                        kx[h, r0 : r0 + span], q, (((1,), (1,)), ((), ())),
                        preferred_element_type=F32,
                    )
                    sc = sc + bias[b]
                    top = jnp.maximum(jnp.max(sc, axis=0, keepdims=True), sink)
                    e = jnp.exp(sc - top)
                    total = jnp.sum(e, axis=0, keepdims=True) + jnp.exp(sink - top)
                    v0 = kw + (h // group) * HEAD_DIM - vfirst
                    o = jnp.dot(
                        vt[v0 : v0 + HEAD_DIM, r0 : r0 + span], e.astype(BF16),
                        preferred_element_type=F32,
                    )
                    outs.append(o / total)
                    lst[s, h : h + 1, r0 : r0 + ar] = top + jnp.log(total)
                both = jnp.concatenate(outs, axis=0).T
                gbuf[s, r0 : r0 + ar, pair * LANES : (pair + 1) * LANES] = both.astype(BF16)

    def activate(s):
        parts = [xm[token_rows(s), t * step : t * step + ch].astype(F32) for t in range(tp)]
        mean = sum(p.sum(-1, keepdims=True) for p in parts) / (tp * ch)
        parts = [p - mean for p in parts]
        var = sum((p * p).sum(-1, keepdims=True) for p in parts) / (tp * ch)
        inv = lax.rsqrt(var + EPSILON)
        for t in range(tp):
            v = parts[t] * inv * gains[t, 0:1]
            xm[token_rows(s), t * step : t * step + ch] = jax.nn.silu(v).astype(BF16)

    def gain_copy(e, landing):
        other = lax.rem(ti + tp - e, tp) if landing else lax.rem(ti + e, tp)
        dst = gains.at[other if landing else ti]
        return remote(gsend, dst, gs.at[e], gr.at[e], {"tp": other})

    assert ch == qw
    fill_bias()
    halo_clear()
    outs = range(2, len(lanes))

    def poll_all(d):
        if d < nz:
            for lane in outs:
                lane_poll(lane, d)

    def partner_start(k):
        partner_all(lambda lane, k, p: None if p else partner(lane, k, p, False).start(), (k,))

    cuts = [0] + [blocks * (3 + 2 * k) // 8 for k in range(nz - 1)] + [blocks]
    cuts = [min(k, blocks) for k in cuts]
    for k in range(nz):
        lax.fori_loop(cuts[k], cuts[k + 1], norm_block, 0)
        if k < nz - 1:
            lane_poll(0, k + 1)
        if k == 0:
            for e in range(1, tp):
                gain_copy(e, False).start()
        if k == min(1, nz - 2):
            hop_start(1)
    fan_start(1)
    for p in range(1, nx):
        exchange(0, p, False).start()
    lane_settle(0)
    def second(d):
        if d < nz:
            lane_poll(1, d)

    nothing = lambda: None
    project(0, finish_gated, [nothing, lambda: second(1), nothing, lambda: second(2)])

    def exchanged():
        for p in range(1, nx):
            exchange(0, p, True).wait_recv()
        for p in range(1, ny):
            exchange(1, p, True).wait_recv()
        for lane in outs:
            fan_start(lane)
            hop_start(lane)

    def late_second():
        for d in range(3, nz):
            second(d)

    def dw_step(s, carry):
        when(s == min(1, seqs - 1), late_second)
        when(s == min(2, seqs - 1), exchanged)
        return depthwise(s, carry)

    lax.fori_loop(0, seqs, dw_step, 0)
    lane_settle(1)
    project(1, finish_qkv, [nothing, lambda: poll_all(1)])
    partner_start(0)
    for e in range(1, tp):
        gain_copy(e, True).wait_recv()
    for s in range(seqs):
        halo_drain(0, s)

    def attend_step(s, carry):
        halo_wait(1, s)
        attend(s)
        scatter_start(1, s)
        scatter_wait(0, s)
        activate(s)
        for d in range(2, nz):
            when(s == min(d - 2, seqs - 1), lambda d=d: poll_all(d))

        def share_most():
            for k in range(1, arrivals):
                partner_start(k)

        when(s == min(max(1, nz - 3), seqs - 1), share_most)
        return carry

    lax.fori_loop(0, seqs, attend_step, 0)
    log_copy = pltpu.make_async_copy(lst, log_ref, log_sem.at[0])
    log_copy.start()
    for lane in outs:
        lane_settle(lane)
    partner_all(lambda lane, k, p: partner(lane, k, p, False).start() if p else None, range(arrivals))
    for s in range(seqs):
        scatter_wait(1, s)
    partner_all(lambda lane, k, p: partner(lane, k, p, True).wait_recv(), range(arrivals))

    def out_copy(j):
        slot = lax.rem(j, 2)
        dst = mixed_ref.at[:, :, pl.ds(pl.multiple_of(j * cols, cols), cols)]
        return pltpu.make_async_copy(stage_out.at[slot], dst, out_sem.at[slot])

    def out_step(j, carry):
        @pl.when(j >= 2)
        def _():
            out_copy(j - 2).wait()

        v = jnp.dot(xm[...], wo[j], preferred_element_type=F32).astype(BF16)
        stage_out[lax.rem(j, 2)] = v.reshape(seqs, share, cols)
        out_copy(j).start()
        return carry

    lax.fori_loop(0, sp, out_step, 0)

    for lane in range(len(lanes)):
        lane_drain(lane)
    for p in range(1, nx):
        exchange(0, p, False).wait_send()
    for p in range(1, ny):
        exchange(1, p, False).wait_send()
    partner_all(lambda lane, k, p: partner(lane, k, p, False).wait_send(), range(arrivals))
    for e in range(1, tp):
        gain_copy(e, False).wait_send()
    for s in range(seqs):
        halo_drain(1, s)
    for b in range(2):
        for s in range(seqs):
            for e in range(1, tp):
                scatter(b, s, e, False).wait_send()
    log_copy.wait()
    for j in range(max(sp - 2, 0), sp):
        out_copy(j).wait()


def mega(tokens, norm_gain, taps, conv_gain, sink, conv_shards, qkv_shards, out_shards, qw, kw):
    seqs, tok, width = tokens.shape
    tp, sp = lax.axis_size("tp"), lax.axis_size("sp")
    nz, nx = grid_of(sp)
    nc = 2 if tp % 2 == 0 else 1
    ny = tp // nc
    rows = seqs * tok
    taps_n, ch = taps.shape
    kd = width // sp
    halo = -(-(taps_n // 2) // 16) * 16
    rb = math.gcd(tok, TOKB)
    share = tok // tp
    heads = qw // HEAD_DIM
    group = heads // (kw // HEAD_DIM)
    cols = out_shards[0].shape[1]
    step = ch + qw
    tables, sign = rope_tables(tok, sp)
    dims = (
        sp, nz, nx, ny, nc, seqs, tok, tp, ch, qw, kw, taps_n, halo, group,
        len(conv_shards), len(qkv_shards),
    )
    vmem = pl.BlockSpec(memory_space=pltpu.VMEM)
    hbm = pl.BlockSpec(memory_space=pl.ANY)
    n = qw + 2 * kw
    pieces = len(conv_shards) + len(qkv_shards) + 2
    ar = math.gcd(share, 256)
    span = ar + 2 * WINDOW
    length = tok + 2 * WINDOW
    vfirst = kw // LANES * LANES
    lanes = 2 + nx + ny
    dma = pltpu.SemaphoreType.DMA
    per_lane = (2 * nz - 1) * PEERS
    return pl.pallas_call(
        functools.partial(mega_kernel, dims),
        in_specs=[hbm] + [vmem] * 8 + [pl.BlockSpec(memory_space=pltpu.SMEM)] + [hbm] * pieces,
        out_specs=[hbm] * 2,
        out_shape=[
            jax.ShapeDtypeStruct((seqs, share, width), BF16),
            jax.ShapeDtypeStruct((seqs, heads, tok), F32),
        ],
        scratch_shapes=[
            pltpu.VMEM((SLOTS, rb, width), BF16),
            pltpu.VMEM((rows, width), BF16),
            pltpu.VMEM((width, 2 * ch), BF16),
            pltpu.VMEM((width, n), BF16),
            pltpu.VMEM((sp, tp * step, cols), BF16),
            pltpu.VMEM((seqs, tok, ch), BF16),
            pltpu.VMEM((seqs, halo, ch), BF16),
            pltpu.VMEM((seqs, halo, ch), BF16),
            pltpu.VMEM((tok + 2 * halo, ch), F32),
            pltpu.VMEM((tp, seqs, share, ch), BF16),
            pltpu.VMEM((seqs, tok, qw), BF16),
            pltpu.VMEM((seqs, tok, 2 * kw), BF16),
            pltpu.VMEM((seqs, WINDOW, 2 * kw), BF16),
            pltpu.VMEM((seqs, WINDOW, 2 * kw), BF16),
            pltpu.VMEM((length, 2 * kw), BF16),
            pltpu.VMEM((heads, length, LANES), BF16),
            pltpu.VMEM((2 * kw - vfirst, length), BF16),
            pltpu.VMEM((tok // ar, span, ar), F32),
            pltpu.VMEM((seqs, heads, tok), F32),
            pltpu.VMEM((seqs * share, tp * step), BF16),
            pltpu.VMEM((2, seqs, share, cols), BF16),
            pltpu.VMEM((tok, LANES), F32),
            pltpu.VMEM((tok, LANES), F32),
            pltpu.VMEM((1, width), F32),
            pltpu.VMEM((taps_n, ch), F32),
            pltpu.VMEM((8, ch), F32),
            pltpu.VMEM((tp, 8, ch), F32),
            dma((SLOTS,)),
            dma((2, max(len(conv_shards), len(qkv_shards)))),
            dma((2,)),
            dma((lanes, 2, nz)),
            dma((lanes, 2, nz)),
            dma((lanes, per_lane)),
            dma((lanes, per_lane)),
            dma((2, PEERS)),
            dma((2, PEERS)),
            dma((lanes, per_lane)),
            dma((lanes, per_lane)),
            dma((2, 2, seqs)),
            dma((2, 2, seqs)),
            dma((2, seqs, tp)),
            dma((2, seqs, tp)),
            dma((2, seqs)),
            dma((tp,)),
            dma((tp,)),
            dma((2,)),
            dma((1,)),
        ],
        compiler_params=pltpu.CompilerParams(
            vmem_limit_bytes=VMEM_LIMIT, collective_id=0, has_side_effects=True
        ),
        cost_estimate=cost(6 * rows * width * (n + 2 * ch), 4 * rows * width),
        name="layer",
    )(
        tokens.reshape(rows, width),
        norm_gain,
        *tables,
        sign,
        taps,
        conv_gain,
        sink,
        *conv_shards,
        *qkv_shards,
        *out_shards,
    )


def on_device(
    tokens,
    norm_gain,
    conv_value_weight,
    conv_gate_weight,
    query_weight,
    key_weight,
    value_weight,
    conv_taps,
    conv_gain,
    sink_logit,
    out_conv_weight,
    out_attn_weight,
):
    qw, kw = query_weight.shape[1], key_weight.shape[1]
    qkv_shards = [query_weight, key_weight, value_weight]
    if kw % LANES:
        qkv_shards[1:] = [jnp.concatenate(qkv_shards[1:], 1)]
    mixed, log_total = mega(
        tokens,
        norm_gain,
        conv_taps,
        conv_gain,
        sink_logit,
        [conv_value_weight, conv_gate_weight],
        qkv_shards,
        [out_conv_weight, out_attn_weight],
        qw,
        kw,
    )
    return (mixed, log_total)


def solution(mesh):
    placed = (
        P(None, "sp", None),
        P(),
        P("sp", "tp"),
        P("sp", "tp"),
        P("sp", "tp"),
        P("sp", "tp"),
        P("sp", "tp"),
        P(None, "tp"),
        P("tp"),
        P("tp"),
        P("tp", "sp"),
        P("tp", "sp"),
    )
    return jax.shard_map(
        on_device,
        mesh=mesh,
        in_specs=placed,
        out_specs=(P(None, ("sp", "tp"), None), P(None, "tp", "sp")),
        check_vma=False,
    )
```
